32 devices in a mesh: ep: 8 (over z, y), tp: 4 (over x, core).
Axes of the slice: x: 2, y: 2, z: 4, core: 2. Of those that a mesh axis runs over, the one named last changes fastest.
Arguments:
- tokens: bfloat16 [192, 2048], P('ep'), may hold values from -6 to 6
- delta_state: float32 [192, 8, 128, 128], P('ep', 'tp'), may hold values from -3 to 3
- first_gain: bfloat16 [2048], replicated, may hold values from 0.099609375 to 1.8984375
- query_weight: bfloat16 [2048, 1024], P(None, 'tp'), may hold values from -0.125 to 0.125
- key_weight: bfloat16 [2048, 1024], P(None, 'tp'), may hold values from -0.125 to 0.125
- value_weight: bfloat16 [2048, 1024], P(None, 'tp'), may hold values from -0.125 to 0.125
- outgate_weight: bfloat16 [2048, 1024], P(None, 'tp'), may hold values from -0.125 to 0.125
- beta_weight: bfloat16 [2048, 8], replicated, may hold values from -0.125 to 0.125
- decay_weight: bfloat16 [2048, 8], replicated, may hold values from -0.125 to 0.125
- decay_rate: float32 [8], replicated, may hold values from 0.05 to 4
- decay_bias: float32 [8], replicated, may hold values from -3 to 3
- head_gain: bfloat16 [128], replicated, may hold values from 0.099609375 to 1.8984375
- out_weight: bfloat16 [1024, 2048], P('tp'), may hold values from -0.1875 to 0.1875
- second_gain: bfloat16 [2048], replicated, may hold values from 0.099609375 to 1.8984375
- blend_weight: bfloat16 [2048], replicated, may hold values from -0.125 to 0.125
- dense_gate_weight: bfloat16 [2048, 2048], P(None, 'tp'), may hold values from -0.125 to 0.125
- dense_up_weight: bfloat16 [2048, 2048], P(None, 'tp'), may hold values from -0.125 to 0.125
- dense_down_weight: bfloat16 [2048, 2048], P('tp'), may hold values from -0.125 to 0.125
- expert_gate: bfloat16 [32, 2048, 512], P(('ep', 'tp')), may hold values from -0.125 to 0.125
- expert_up: bfloat16 [32, 2048, 512], P(('ep', 'tp')), may hold values from -0.125 to 0.125
- expert_down: bfloat16 [32, 512, 2048], P(('ep', 'tp')), may hold values from -0.25 to 0.25
- route_ids: int32 [192, 6], P('ep'), may hold values from 0 to 31, all different within a row; in each aligned block of 24 rows (0 to 23, 24 to 47, ...) at most 7 rows name the same one
- route_weights: float32 [192, 6], P('ep'), may hold values from 0.1 to 1
Outputs:
- new_tokens: bfloat16 [192, 2048], P('ep')
- new_state: float32 [192, 8, 128, 128], P('ep', 'tp')
The draws below stay inside these ranges and needn't reach their ends.
Inputs may be any that keep to these rules, and one draw needn't show every extreme that they name: `route_ids`: each row names 6 different experts. In each aligned block of 24 rows (the sequences of one index of ep) no expert is named by more than 7 rows, and in some block an expert is named by exactly 7 rows.
All inputs are finite; a program needn't handle non-finite values.
Results may differ from the reference program's by a relative error of at most 0.017.
Values may be sent and summed in bfloat16 or wider, within the bound.
A program may use at most 128 MiB of HBM per device.

```python
import math
import jax
import jax.numpy as jnp
import numpy as np
from jax import lax

D = 2048
HEADS = 8
HD = 128
DFF = 2048
DE = 512
TOP_K = 6
SEQ_DEV = 24
TOKENS = 192
EXPERTS = 32
CAP = 7
N_EP = 8


def block_levels(rng, shape, cuts, low, high):
    def one(position, shards_of):
        draws = jax.random.uniform(jax.random.fold_in(jax.random.fold_in(rng, 6), position), (shards_of,), jnp.float32, low / len(cuts), high / len(cuts))
        return jnp.repeat(jnp.exp(draws), shape[position] // shards_of).reshape((-1,) + (1,) * (len(shape) - position - 1))

    loudness = one(*cuts[0])
    for cut in cuts[1:]:
        loudness = loudness * one(*cut)
    return loudness


def shared_out(rng, own, number, rows, number_of, top, reach, lean):
    ranking = jax.random.permutation(rng, number_of)
    crowded, common = shares(number_of, rows * top, reach, lean, True), shares(number_of, rows * top, reach, lean, False)
    places = jnp.arange(number_of)

    def named(sizes, turn):
        used = int((sizes > 0).sum())
        fixed = max(1, used // 4)
        passed = fixed + (places - fixed + turn * (used - fixed)) % max(1, number_of - fixed)
        return jnp.zeros((number_of,), jnp.int32).at[ranking[jnp.where(places < fixed, places, passed)]].set(jnp.asarray(sizes, jnp.int32))

    sizes = jnp.where(number % 4 == 0, named(crowded, number // 4), named(common, number - number // 4 - 1))
    mixed = jax.random.permutation(jax.random.fold_in(own, 3), number_of)
    donor, taker = mixed[0:number_of // 2 * 2:2], mixed[1:number_of // 2 * 2:2]
    margin = jnp.minimum(sizes[donor] - 1, reach - sizes[taker]) // 2
    margin = jnp.where((donor == ranking[0]) | (taker == ranking[0]) | (sizes[taker] == 0), 0, jnp.maximum(margin, 0))
    passed = jax.random.randint(jax.random.fold_in(own, 4), (number_of // 2,), 0, 1 << 20) % (margin + 1)
    sizes = sizes.at[donor].add(-passed).at[taker].add(passed)
    members = jnp.searchsorted(jnp.cumsum(sizes), jnp.arange(rows * top), side="right").astype(jnp.int32)
    listing = members.reshape(top, rows).T
    listing = listing[jax.random.permutation(jax.random.fold_in(own, 1), rows)]
    turn = jax.random.randint(jax.random.fold_in(own, 2), (rows, 1), 0, top)
    return jnp.take_along_axis(listing, (jnp.arange(top)[None, :] + turn) % top, axis=1)


def shares(amount, total, reach, lean, full):
    loads = [(1 << 20) // math.isqrt(standing ** lean) + 1 for standing in range(1, amount + 1)]
    largest = reach if full else min(reach, max(-(-total // amount), total * loads[0] // sum(loads)))
    least = 1 if total - largest >= amount - 1 else 0
    holding, spare = [largest] + [least] * (amount - 1), total - largest - least * (amount - 1)
    while spare > 0:
        movable = [i for i in range(1, amount) if holding[i] < largest] or [i for i in range(1, amount) if holding[i] < reach]
        mass, left = sum([loads[i] for i in movable]), spare
        for i in movable:
            extra = min(reach - holding[i], max(1, left * loads[i] // mass), spare)
            holding[i] = holding[i] + extra
            spare = spare - extra
    return np.array(holding)


def scatter_about(key, dims, spread, limit, pieces=(), kind=jnp.bfloat16):
    factor_of = block_levels(key, dims, pieces, -0.22, 0.18) if pieces else 1.0
    array = jax.random.normal(key, dims, jnp.float32) * spread * factor_of
    return jnp.minimum(jnp.maximum(array, -limit), limit).astype(kind)


def setup_inputs(seed: int = 0) -> dict:
    key_list = jax.random.split(jax.random.key(seed), 24)
    tokens = scatter_about(key_list[0], (TOKENS, D), 1.0, 6.0, ((0, 8),))
    delta_state = scatter_about(key_list[1], (TOKENS, HEADS, HD, HD), 0.3, 3.0, ((0, 8), (1, 4)), jnp.float32)
    first_gain = jnp.clip(1.0 + 0.18 * jax.random.normal(key_list[2], (D,), jnp.float32), 0.099609375, 1.8984375).astype(jnp.bfloat16)
    query_weight = scatter_about(key_list[3], (D, HEADS * HD), D ** -0.5, 0.125, ((1, 4),))
    key_weight = scatter_about(key_list[4], (D, HEADS * HD), D ** -0.5, 0.125, ((1, 4),))
    value_weight = scatter_about(key_list[5], (D, HEADS * HD), D ** -0.5, 0.125, ((1, 4),))
    outgate_weight = scatter_about(key_list[6], (D, HEADS * HD), D ** -0.5, 0.125, ((1, 4),))
    beta_weight = scatter_about(key_list[7], (D, HEADS), D ** -0.5, 0.125)
    decay_weight = scatter_about(key_list[8], (D, HEADS), D ** -0.5, 0.125)
    decay_rate = jnp.clip(jnp.exp(jax.random.uniform(key_list[9], (HEADS,), jnp.float32, math.log(0.05), math.log(4.0))), 0.05, 4.0)
    decay_bias = scatter_about(key_list[10], (HEADS,), 1.0, 3.0, (), jnp.float32)
    head_gain = jnp.clip(1.0 + 0.18 * jax.random.normal(key_list[11], (HD,), jnp.float32), 0.099609375, 1.8984375).astype(jnp.bfloat16)
    out_weight = scatter_about(key_list[12], (HEADS * HD, D), (HEADS * HD) ** -0.5, 0.1875, ((0, 4),))
    second_gain = jnp.clip(1.0 + 0.18 * jax.random.normal(key_list[13], (D,), jnp.float32), 0.099609375, 1.8984375).astype(jnp.bfloat16)
    blend_weight = scatter_about(key_list[14], (D,), D ** -0.5, 0.125)
    dense_gate_weight = scatter_about(key_list[15], (D, DFF), D ** -0.5, 0.125, ((1, 4),))
    dense_up_weight = scatter_about(key_list[16], (D, DFF), D ** -0.5, 0.125, ((1, 4),))
    dense_down_weight = scatter_about(key_list[17], (DFF, D), DFF ** -0.5, 0.125, ((0, 4),))
    expert_gate = scatter_about(key_list[18], (EXPERTS, D, DE), D ** -0.5, 0.125, ((0, 32),))
    expert_up = scatter_about(key_list[19], (EXPERTS, D, DE), D ** -0.5, 0.125, ((0, 32),))
    expert_down = scatter_about(key_list[20], (EXPERTS, DE, D), DE ** -0.5, 0.25, ((0, 32),))
    route_ids_keys = jax.random.split(jax.random.fold_in(key_list[21], 1), TOKENS // SEQ_DEV)
    route_ids_turns = jax.random.permutation(jax.random.fold_in(key_list[21], 3), TOKENS // SEQ_DEV)
    route_ids = jax.vmap(lambda own, number: shared_out(jax.random.fold_in(key_list[21], 2), own, number, SEQ_DEV, EXPERTS, TOP_K, CAP, 2))(route_ids_keys, route_ids_turns).reshape((TOKENS, TOP_K))
    route_weights = jnp.clip(jnp.exp(math.log(1.0) - 2.3025851 * jax.random.uniform(key_list[22], (TOKENS, TOP_K), jnp.float32) ** block_levels(key_list[22], (TOKENS, TOP_K), ((0, 8),), -0.2, 0.2)), 0.1, 1.0)
    return {"tokens": tokens, "delta_state": delta_state, "first_gain": first_gain, "query_weight": query_weight, "key_weight": key_weight, "value_weight": value_weight, "outgate_weight": outgate_weight, "beta_weight": beta_weight, "decay_weight": decay_weight, "decay_rate": decay_rate, "decay_bias": decay_bias, "head_gain": head_gain, "out_weight": out_weight, "second_gain": second_gain, "blend_weight": blend_weight, "dense_gate_weight": dense_gate_weight, "dense_up_weight": dense_up_weight, "dense_down_weight": dense_down_weight, "expert_gate": expert_gate, "expert_up": expert_up, "expert_down": expert_down, "route_ids": route_ids, "route_weights": route_weights}


norm_eps = 1e-06
unit_eps = 1e-06
routed_scale = 2.5

def rms_scale(values, gain):
    values = values.astype(jnp.float32)
    inverse = lax.rsqrt(lax.optimization_barrier(jnp.mean(values * values, axis=-1, keepdims=True)) + norm_eps)
    return values * inverse * gain.astype(jnp.float32)

def unit_rows(values):
    return values * lax.rsqrt(lax.optimization_barrier(jnp.sum(values * values, axis=-1, keepdims=True)) + unit_eps)

def rounded(values):
    return lax.optimization_barrier(values.astype(jnp.bfloat16)).astype(jnp.float32)

def delta_update(delta_state, query_raw, key_raw, value_raw, beta_gate, log_decay):
    head_size = delta_state.shape[-1]
    query_unit = unit_rows(jax.nn.silu(query_raw)) * head_size ** (-0.5)
    key_unit = unit_rows(jax.nn.silu(key_raw))
    value_act = jax.nn.silu(value_raw)
    decayed = jnp.exp(log_decay)[:, :, None, None] * delta_state
    predicted = jnp.einsum('shkv,shk->shv', decayed, key_unit, precision=lax.Precision.HIGHEST)
    update = (beta_gate[:, :, None] * key_unit)[:, :, :, None] * (value_act - predicted)[:, :, None, :]
    new_state = decayed + update
    readout = jnp.einsum('shkv,shk->shv', new_state, query_unit, precision=lax.Precision.HIGHEST)
    return (new_state, readout)

def gated_heads(readout, outgate_raw, head_gain):
    scaled = rms_scale(readout, head_gain) * jax.nn.silu(outgate_raw)
    return scaled.reshape(scaled.shape[0], -1).astype(jnp.bfloat16)

def expert_rows(row_block, gate_mat, up_mat, down_mat):
    gate_part = jnp.dot(row_block, gate_mat, preferred_element_type=jnp.float32)
    up_part = jnp.dot(row_block, up_mat, preferred_element_type=jnp.float32)
    hidden = (jax.nn.silu(gate_part) * up_part).astype(jnp.bfloat16)
    return jnp.dot(hidden, down_mat, preferred_element_type=jnp.float32).astype(jnp.bfloat16)

def routed_sum(normed_mid, expert_gate, expert_up, expert_down, route_ids, route_scale):
    seq_count, model_width = normed_mid.shape
    top_count = route_ids.shape[1]
    per_group = SEQ_DEV * top_count
    grouped = route_ids.reshape(N_EP, per_group).astype(jnp.int32)
    earlier = jnp.arange(per_group)[:, None] > jnp.arange(per_group)[None, :]
    matches = (grouped[:, :, None] == grouped[:, None, :]) & earlier[None]
    rank_of = lax.optimization_barrier(jnp.sum(matches.astype(jnp.int32), axis=2))
    group_ids = jnp.arange(N_EP, dtype=jnp.int32)[:, None]
    expert_slots = N_EP * CAP
    slot_ids = (grouped * expert_slots + group_ids * CAP + rank_of).reshape(-1).astype(jnp.int32)
    token_ids = jnp.arange(seq_count * top_count, dtype=jnp.int32) // top_count
    slot_table = jnp.zeros((EXPERTS * expert_slots,), jnp.int32).at[slot_ids].set(token_ids + 1)
    padded = jnp.concatenate([jnp.zeros((1, model_width), normed_mid.dtype), normed_mid], axis=0)

    def one_expert(inputs):
        index_row, gate_mat, up_mat, down_mat = inputs
        return expert_rows(padded[index_row], gate_mat, up_mat, down_mat)
    outputs = lax.map(one_expert, (slot_table.reshape(EXPERTS, expert_slots), expert_gate, expert_up, expert_down))
    picked = outputs.reshape(-1, model_width)[slot_ids].astype(jnp.float32)
    picked = picked.reshape(seq_count, top_count, model_width)
    return lax.optimization_barrier(jnp.sum(route_scale[:, :, None] * picked, axis=1))

def reference(tokens, delta_state, first_gain, query_weight, key_weight, value_weight, outgate_weight, beta_weight, decay_weight, decay_rate, decay_bias, head_gain, out_weight, second_gain, blend_weight, dense_gate_weight, dense_up_weight, dense_down_weight, expert_gate, expert_up, expert_down, route_ids, route_weights):
    seq_count = tokens.shape[0]
    normed = rms_scale(tokens, first_gain).astype(jnp.bfloat16)

    def project(weight):
        product = jnp.dot(normed, weight, preferred_element_type=jnp.float32)
        return rounded(product).reshape(seq_count, HEADS, HD)
    query_raw = project(query_weight)
    key_raw = project(key_weight)
    value_raw = project(value_weight)
    outgate_raw = project(outgate_weight)
    beta_gate = jax.nn.sigmoid(jnp.dot(normed, beta_weight, preferred_element_type=jnp.float32))
    decay_input = jnp.dot(normed, decay_weight, preferred_element_type=jnp.float32) + decay_bias
    log_decay = -decay_rate * jax.nn.softplus(decay_input)
    new_state, readout = delta_update(delta_state, query_raw, key_raw, value_raw, beta_gate, log_decay)
    gated = gated_heads(readout, outgate_raw, head_gain)
    mixed = jnp.dot(gated, out_weight, preferred_element_type=jnp.float32)
    residual = (tokens.astype(jnp.float32) + mixed).astype(jnp.bfloat16)
    normed_mid = rms_scale(residual, second_gain).astype(jnp.bfloat16)
    blend_gate = jax.nn.sigmoid(jnp.dot(normed_mid, blend_weight, preferred_element_type=jnp.float32))
    dense_gate_raw = jnp.dot(normed_mid, dense_gate_weight, preferred_element_type=jnp.float32)
    dense_up_raw = jnp.dot(normed_mid, dense_up_weight, preferred_element_type=jnp.float32)
    dense_hidden = (jax.nn.silu(dense_gate_raw) * dense_up_raw).astype(jnp.bfloat16)
    dense_out = jnp.dot(dense_hidden, dense_down_weight, preferred_element_type=jnp.float32)
    route_scale = route_weights / lax.optimization_barrier(jnp.sum(route_weights, axis=1, keepdims=True)) * routed_scale
    routed = routed_sum(normed_mid, expert_gate, expert_up, expert_down, route_ids, route_scale)
    combined = residual.astype(jnp.float32) + routed + blend_gate[:, None] * dense_out
    return (combined.astype(jnp.bfloat16), new_state)
```

```python
import functools

import jax
import jax.numpy as jnp
from jax import lax
from jax.experimental import pallas as pl
from jax.experimental.pallas import tpu as pltpu
from jax.sharding import PartitionSpec as P

norm_eps = 1e-06
unit_eps = 1e-06
routed_scale = 2.5
vmem_bytes = 60 * 1024 * 1024
MESH = pl.DeviceIdType.MESH
f32 = jnp.float32
bf16 = jnp.bfloat16


def rms_scale(values, gain):
    inverse = lax.rsqrt(jnp.mean(values * values, axis=-1, keepdims=True) + norm_eps)
    return values * inverse * gain


def unit_rows(values):
    return values * lax.rsqrt(jnp.sum(values * values, axis=-1, keepdims=True) + unit_eps)


def silu(values):
    return values * jax.nn.sigmoid(values)


def dot(left, right):
    return jnp.dot(left, right, preferred_element_type=f32)


def mixer_kernel(
    seq_chunk,
    tokens_ref,
    gain_ref,
    head_gain_ref,
    rate_ref,
    bias_ref,
    query_hbm,
    key_hbm,
    value_hbm,
    outgate_hbm,
    beta_hbm,
    decay_hbm,
    out_hbm,
    state_hbm,
    mix_ref,
    new_state_hbm,
    proj_buf,
    beta_buf,
    decay_buf,
    out_buf,
    state_buf,
    column_buf,
    readout_buf,
    proj_sem,
    gate_sem,
    out_sem,
    state_sem,
    store_sem,
):
    seq_count = tokens_ref.shape[0]
    head_local, head_size = state_buf.shape[1:3]
    width = head_local * head_size
    chunk_count = seq_count // seq_chunk
    gate_copies = [
        pltpu.make_async_copy(beta_hbm, beta_buf, gate_sem.at[0]),
        pltpu.make_async_copy(decay_hbm, decay_buf, gate_sem.at[1]),
    ]
    proj_copies = [
        pltpu.make_async_copy(hbm, proj_buf.at[i], proj_sem.at[i])
        for i, hbm in enumerate((key_hbm, query_hbm, value_hbm, outgate_hbm))
    ]
    chunks = [pl.ds(c * seq_chunk, seq_chunk) for c in range(chunk_count)]
    state_copies = [
        pltpu.make_async_copy(state_hbm.at[rows], state_buf.at[rows], state_sem.at[c])
        for c, rows in enumerate(chunks)
    ]
    store_copies = [
        pltpu.make_async_copy(state_buf.at[rows], new_state_hbm.at[rows], store_sem.at[c])
        for c, rows in enumerate(chunks)
    ]
    out_copy = pltpu.make_async_copy(out_hbm, out_buf, out_sem.at[0])
    for copy in proj_copies[:3] + gate_copies + state_copies + proj_copies[3:] + [out_copy]:
        copy.start()

    normed = rms_scale(tokens_ref[...].astype(f32), gain_ref[...].astype(f32)).astype(bf16)

    def project(index):
        proj_copies[index].wait()
        return dot(normed, proj_buf[index]).astype(bf16).astype(f32)

    def heads_of(raw):
        return [raw[:, h * head_size : (h + 1) * head_size] for h in range(head_local)]

    key_units = [unit_rows(silu(raw)) for raw in heads_of(project(0))]
    query_units = [
        unit_rows(silu(raw)) * head_size ** (-0.5) for raw in heads_of(project(1))
    ]
    value_acts = [silu(raw) for raw in heads_of(project(2))]
    for copy in gate_copies:
        copy.wait()
    beta_all = jax.nn.sigmoid(dot(normed, beta_buf[...]))
    decay_all = dot(normed, decay_buf[...])
    lane = lax.broadcasted_iota(jnp.int32, beta_all.shape, 1)
    head_start = lax.axis_index("tp") * head_local
    betas, alphas = [], []
    for h in range(head_local):
        chosen = lane == head_start + h
        betas.append(jnp.sum(jnp.where(chosen, beta_all, 0.0), axis=1, keepdims=True))
        raw = jnp.sum(jnp.where(chosen, decay_all, 0.0), axis=1, keepdims=True)
        raw = raw + bias_ref[head_start + h]
        soft = jnp.maximum(raw, 0.0) + jnp.log1p(jnp.exp(-jnp.abs(raw)))
        alphas.append(jnp.exp(-rate_ref[head_start + h] * soft))
    wide = (seq_count, head_size)
    betas = [jnp.broadcast_to(beta, wide) for beta in betas]
    alphas = [jnp.broadcast_to(alpha, wide) for alpha in alphas]
    stacked = jnp.concatenate(key_units + query_units, axis=0)
    short = -stacked.shape[0] % head_size
    if short:
        stacked = jnp.concatenate([stacked, jnp.zeros((short, head_size), f32)], axis=0)
    column_buf[...] = stacked.T
    for c in range(chunk_count):
        state_copies[c].wait()
        for s in range(c * seq_chunk, (c + 1) * seq_chunk):
            for h in range(head_local):
                key_at = h * seq_count + s
                query_at = (head_local + h) * seq_count + s
                key_column = column_buf[:, key_at : key_at + 1]
                query_column = column_buf[:, query_at : query_at + 1]
                alpha = alphas[h][s : s + 1]
                old = state_buf[s, h]
                predicted = alpha * jnp.sum(old * key_column, axis=0, keepdims=True)
                change = betas[h][s : s + 1] * (value_acts[h][s : s + 1] - predicted)
                new = old * alpha + key_column * change
                state_buf[s, h] = new
                readout_buf[s : s + 1, h * head_size : (h + 1) * head_size] = jnp.sum(
                    new * query_column, axis=0, keepdims=True
                )
        store_copies[c].start()
    outgate = project(3)
    gain = head_gain_ref[...].astype(f32)
    gated = [rms_scale(part, gain) for part in heads_of(readout_buf[...])]
    gated = (jnp.concatenate(gated, axis=1) * silu(outgate)).astype(bf16)
    out_copy.wait()
    half = mix_ref.shape[2]
    for i in range(mix_ref.shape[0]):
        mix_ref[i] = dot(gated, out_buf[:, i * half : (i + 1) * half]).astype(bf16)
    for copy in store_copies:
        copy.wait()


def expert_kernel(
    ep_count,
    tp_count,
    capacity,
    mix_ref,
    tokens_ref,
    gain_ref,
    blend_ref,
    ids_ref,
    weights_ref,
    dense_gate_hbm,
    dense_up_hbm,
    dense_down_hbm,
    gate_hbm,
    up_hbm,
    down_hbm,
    out_ref,
    wide_buf,
    dense_down_buf,
    down_buf,
    pair_buf,
    chip_buf,
    cross_buf,
    residual_buf,
    part_buf,
    pair_two_buf,
    chip_two_buf,
    cross_two_buf,
    final_buf,
    outgoing_buf,
    arrived_buf,
    result_buf,
    returned_buf,
    rows_buf,
    weight_sem,
    tp_send,
    tp_recv,
    ep_send,
    ep_recv,
):
    seq_count, width = tokens_ref.shape
    half = width // 2
    slot_rows = outgoing_buf.shape[1]
    me = lax.axis_index("ep")
    tp_index = lax.axis_index("tp")
    core = lax.rem(tp_index, 2)
    chip = tp_index // 2
    partner = chip * 2 + 1 - core
    across = lax.rem(chip + 1, 2) * 2 + core

    weight_copies = [
        pltpu.make_async_copy(hbm, buf, weight_sem.at[i])
        for i, (hbm, buf) in enumerate(
            (
                (dense_gate_hbm, wide_buf.at[0]),
                (dense_up_hbm, wide_buf.at[1]),
                (dense_down_hbm, dense_down_buf),
                (gate_hbm.at[0], wide_buf.at[2]),
                (up_hbm.at[0], wide_buf.at[3]),
                (down_hbm.at[0], down_buf),
            )
        )
    ]
    barrier = pltpu.get_barrier_semaphore()
    pl.semaphore_signal(barrier, inc=1, device_id={"tp": partner}, device_id_type=MESH)
    pl.semaphore_signal(barrier, inc=1, device_id={"tp": across}, device_id_type=MESH)

    def greet(step, carry):
        peer = lax.rem(me + step, ep_count)
        pl.semaphore_signal(barrier, inc=1, device_id={"ep": peer}, device_id_type=MESH)
        return carry

    lax.fori_loop(1, ep_count, greet, 0)
    for copy in weight_copies:
        copy.start()
    pl.semaphore_wait(barrier, ep_count + 1)

    def tp_copy(src, dst, index, target):
        return pltpu.make_async_remote_copy(
            src_ref=src,
            dst_ref=dst,
            send_sem=tp_send.at[index],
            recv_sem=tp_recv.at[index],
            device_id={"tp": target},
            device_id_type=MESH,
        )

    def start_pair(source, pair, base):
        copy = tp_copy(source.at[1 - core], pair, base, partner)
        copy.start()
        return copy

    def finish_sum(copy, source, pair, chip_sum, cross, base):
        copy.wait()
        chip_sum[...] = (source[core].astype(f32) + pair[...].astype(f32)).astype(bf16)
        other = tp_copy(chip_sum, cross, base + 1, across)
        other.start()
        other.wait()
        return chip_sum[...].astype(f32) + cross[...].astype(f32)

    def share(buf, base):
        copy = tp_copy(buf.at[core], buf.at[core], base + 2, partner)
        copy.start()
        tp_copy(buf.at[1 - core], buf.at[1 - core], base + 2, partner).wait_recv()
        copy.wait_send()

    first = start_pair(mix_ref, pair_buf, 0)

    expert_count = ep_count * tp_count
    slot_total = ep_count * slot_rows
    ids = ids_ref[...]
    raw_weights = weights_ref[...]
    scales = raw_weights / jnp.sum(raw_weights, axis=1, keepdims=True) * routed_scale
    expert_lane = lax.broadcasted_iota(jnp.int32, (seq_count, slot_total), 1)
    slot_expert = expert_lane // slot_rows * tp_count + tp_index
    slot_place = lax.rem(expert_lane, slot_rows)
    named = jnp.zeros((seq_count, slot_total), f32)
    scale_at = jnp.zeros((seq_count, slot_total), f32)
    for k in range(ids.shape[1]):
        same = ids[:, k : k + 1] == slot_expert
        named = named + jnp.where(same, 1.0, 0.0)
        scale_at = scale_at + jnp.where(same, scales[:, k : k + 1], 0.0)
    row = lax.broadcasted_iota(jnp.int32, (seq_count, seq_count), 0)
    col = lax.broadcasted_iota(jnp.int32, (seq_count, seq_count), 1)
    earlier = jnp.where(row > col, 1.0, 0.0).astype(bf16)
    rank = dot(earlier, named.astype(bf16))
    taken = named * jnp.where(rank == slot_place.astype(f32), 1.0, 0.0)
    scale_at = scale_at * taken
    scale_high = scale_at.astype(bf16)
    scale_low = (scale_at - scale_high.astype(f32)).astype(bf16)
    dispatch = taken.astype(bf16)

    mixed = finish_sum(first, mix_ref, pair_buf, chip_buf, cross_buf, 0)
    own_tokens = jnp.where(core == 0, tokens_ref[:, :half].astype(f32), tokens_ref[:, half:].astype(f32))
    residual_buf[core] = (own_tokens + mixed).astype(bf16)
    share(residual_buf, 0)
    residual = jnp.concatenate([residual_buf[0], residual_buf[1]], axis=1).astype(f32)
    normed = rms_scale(residual, gain_ref[...].astype(f32)).astype(bf16)
    outgoing = lax.dot_general(
        dispatch, normed, (((0,), (0,)), ((), ())), preferred_element_type=f32
    )
    rows_buf[...] = outgoing

    def fill(peer, carry):
        block = rows_buf[pl.ds(pl.multiple_of(peer * slot_rows, slot_rows), slot_rows), :]
        outgoing_buf[peer] = block.astype(bf16)
        return carry

    lax.fori_loop(0, ep_count, fill, 0, unroll=ep_count <= 8)

    def ep_copy(src, dst, index, src_at, dst_at, target):
        return pltpu.make_async_remote_copy(
            src_ref=src.at[src_at],
            dst_ref=dst.at[dst_at],
            send_sem=ep_send.at[index, src_at],
            recv_sem=ep_recv.at[index, dst_at],
            device_id={"ep": target},
            device_id_type=MESH,
        )

    def send_all(src, dst, index):
        def step_of(step, carry):
            peer = lax.rem(me + step, ep_count)
            ep_copy(src, dst, index, peer, me, peer).start()
            return carry

        lax.fori_loop(1, ep_count, step_of, 0, unroll=ep_count <= 8)
        dst[me] = src[me]

    def wait_all(src, dst, index):
        def step_of(step, carry):
            peer = lax.rem(me + step, ep_count)
            ep_copy(src, dst, index, peer, peer, peer).wait()
            return carry

        lax.fori_loop(1, ep_count, step_of, 0, unroll=ep_count <= 8)

    def gather_rows(buf):
        def step_of(peer, carry):
            at = pl.ds(pl.multiple_of(peer * slot_rows, slot_rows), slot_rows)
            rows_buf[at, :] = buf[peer].astype(f32)
            return carry

        lax.fori_loop(0, ep_count, step_of, 0, unroll=ep_count <= 8)
        return rows_buf[...].astype(bf16)

    send_all(outgoing_buf, arrived_buf, 0)

    blend_row = blend_ref[...].astype(f32)
    blend_gate = jax.nn.sigmoid(
        jnp.sum(normed.astype(f32) * blend_row, axis=1, keepdims=True)
    )
    weight_copies[0].wait()
    dense_gate = dot(normed, wide_buf[0])
    weight_copies[1].wait()
    dense_hidden = (silu(dense_gate) * dot(normed, wide_buf[1])).astype(bf16)
    weight_copies[2].wait()
    dense_part = blend_gate * dot(dense_hidden, dense_down_buf[...])

    wait_all(outgoing_buf, arrived_buf, 0)
    rows = gather_rows(arrived_buf)
    weight_copies[3].wait()
    gate_part = dot(rows, wide_buf[2])
    weight_copies[4].wait()
    hidden = (silu(gate_part) * dot(rows, wide_buf[3])).astype(bf16)
    weight_copies[5].wait()
    rows_buf[...] = dot(hidden, down_buf[...])

    def fill_result(peer, carry):
        block = rows_buf[pl.ds(pl.multiple_of(peer * slot_rows, slot_rows), slot_rows), :]
        result_buf[peer] = block.astype(bf16)
        return carry

    lax.fori_loop(0, ep_count, fill_result, 0, unroll=ep_count <= 8)
    send_all(result_buf, returned_buf, 1)
    wait_all(result_buf, returned_buf, 1)
    rows = gather_rows(returned_buf)
    total = dense_part + dot(scale_high, rows) + dot(scale_low, rows)
    part_buf[0] = total[:, :half].astype(bf16)
    part_buf[1] = total[:, half:].astype(bf16)
    second = start_pair(part_buf, pair_two_buf, 3)
    combined = finish_sum(second, part_buf, pair_two_buf, chip_two_buf, cross_two_buf, 3)
    final_buf[core] = (residual_buf[core].astype(f32) + combined).astype(bf16)
    share(final_buf, 3)
    out_ref[:, :half] = final_buf[0]
    out_ref[:, half:] = final_buf[1]


def shards(
    tokens,
    delta_state,
    first_gain,
    query_weight,
    key_weight,
    value_weight,
    outgate_weight,
    beta_weight,
    decay_weight,
    decay_rate,
    decay_bias,
    head_gain,
    out_weight,
    second_gain,
    blend_weight,
    dense_gate_weight,
    dense_up_weight,
    dense_down_weight,
    expert_gate,
    expert_up,
    expert_down,
    route_ids,
    route_weights,
):
    seq_count, width = tokens.shape
    head_local, head_size = delta_state.shape[1:3]
    ep_count = lax.axis_size("ep")
    tp_count = lax.axis_size("tp")
    half = width // 2
    vmem = pl.BlockSpec(memory_space=pltpu.VMEM)
    smem = pl.BlockSpec(memory_space=pltpu.SMEM)
    hbm = pl.BlockSpec(memory_space=pl.ANY)
    dma = pltpu.SemaphoreType.DMA
    seq_chunk = 4 if seq_count % 4 == 0 else 1
    local_width = query_weight.shape[1]
    stacked = -(-2 * head_local * seq_count // head_size) * head_size
    mix_part, new_state = pl.pallas_call(
        functools.partial(mixer_kernel, seq_chunk),
        out_shape=(
            jax.ShapeDtypeStruct((2, seq_count, half), bf16),
            jax.ShapeDtypeStruct(delta_state.shape, f32),
        ),
        in_specs=[vmem] * 3 + [smem] * 2 + [hbm] * 8,
        out_specs=(vmem, hbm),
        scratch_shapes=[
            pltpu.VMEM((4,) + query_weight.shape, bf16),
            pltpu.VMEM(beta_weight.shape, bf16),
            pltpu.VMEM(decay_weight.shape, bf16),
            pltpu.VMEM(out_weight.shape, bf16),
            pltpu.VMEM(delta_state.shape, f32),
            pltpu.VMEM((head_size, stacked), f32),
            pltpu.VMEM((seq_count, local_width), f32),
            dma((4,)),
            dma((2,)),
            dma((1,)),
            dma((seq_count // seq_chunk,)),
            dma((seq_count // seq_chunk,)),
        ],
        compiler_params=pltpu.CompilerParams(vmem_limit_bytes=vmem_bytes),
        name="mixer",
    )(
        tokens,
        first_gain.reshape(1, -1),
        head_gain.reshape(1, -1),
        decay_rate,
        decay_bias,
        query_weight,
        key_weight,
        value_weight,
        outgate_weight,
        beta_weight,
        decay_weight,
        out_weight,
        delta_state,
    )
    top_count = route_ids.shape[1]
    expert_count = ep_count * tp_count
    capacity = max(2, (3 * seq_count * top_count + 2 * expert_count - 1) // (2 * expert_count))
    slot_rows = -(-capacity // 8) * 8
    wide = pltpu.VMEM((4,) + dense_gate_weight.shape, bf16)
    half_block = pltpu.VMEM((seq_count, half), bf16)
    both_block = pltpu.VMEM((2, seq_count, half), bf16)
    slots = pltpu.VMEM((ep_count, slot_rows, width), bf16)
    new_tokens = pl.pallas_call(
        functools.partial(expert_kernel, ep_count, tp_count, capacity),
        out_shape=jax.ShapeDtypeStruct(tokens.shape, bf16),
        in_specs=[vmem] * 6 + [hbm] * 6,
        out_specs=vmem,
        scratch_shapes=[
            wide,
            pltpu.VMEM(dense_down_weight.shape, bf16),
            pltpu.VMEM(expert_down.shape[1:], bf16),
            half_block,
            half_block,
            half_block,
            both_block,
            both_block,
            half_block,
            half_block,
            half_block,
            both_block,
            slots,
            slots,
            slots,
            slots,
            pltpu.VMEM((ep_count * slot_rows, width), f32),
            dma((6,)),
            dma((6,)),
            dma((6,)),
            dma((2, ep_count)),
            dma((2, ep_count)),
        ],
        compiler_params=pltpu.CompilerParams(
            vmem_limit_bytes=vmem_bytes, collective_id=0, has_side_effects=True
        ),
        name="experts",
    )(
        mix_part,
        tokens,
        second_gain.reshape(1, -1),
        blend_weight.reshape(1, -1),
        route_ids,
        route_weights,
        dense_gate_weight,
        dense_up_weight,
        dense_down_weight,
        expert_gate,
        expert_up,
        expert_down,
    )
    return (new_tokens, new_state)


def solution(mesh):
    placed = (
        P("ep", None),
        P("ep", "tp", None, None),
        P(),
        P(None, "tp"),
        P(None, "tp"),
        P(None, "tp"),
        P(None, "tp"),
        P(),
        P(),
        P(),
        P(),
        P(),
        P("tp", None),
        P(),
        P(),
        P(None, "tp"),
        P(None, "tp"),
        P("tp", None),
        P(("ep", "tp"), None, None),
        P(("ep", "tp"), None, None),
        P(("ep", "tp"), None, None),
        P("ep", None),
        P("ep", None),
    )
    return jax.shard_map(
        shards,
        mesh=mesh,
        in_specs=placed,
        out_specs=(P("ep", None), P("ep", "tp", None, None)),
        check_vma=False,
    )
```

```python
import functools

import jax
import jax.numpy as jnp
from jax import lax
from jax.experimental import pallas as pl
from jax.experimental.pallas import tpu as pltpu
from jax.sharding import PartitionSpec as P

norm_eps = 1e-06
unit_eps = 1e-06
routed_scale = 2.5
vmem_bytes = 60 * 1024 * 1024
MESH = pl.DeviceIdType.MESH
f32 = jnp.float32
bf16 = jnp.bfloat16


def rms_scale(values, gain):
    inverse = lax.rsqrt(jnp.mean(values * values, axis=-1, keepdims=True) + norm_eps)
    return values * inverse * gain


def unit_rows(values):
    return values * lax.rsqrt(jnp.sum(values * values, axis=-1, keepdims=True) + unit_eps)


def silu(values):
    return values * jax.nn.sigmoid(values)


def dot(left, right):
    return jnp.dot(left, right, preferred_element_type=f32)


def dot_t(left, right):
    return lax.dot_general(left, right, (((1,), (1,)), ((), ())), preferred_element_type=f32)


def row_of(ref):
    return ref[...].astype(f32).reshape(1, -1)


def mixer_kernel(
    seq_chunk,
    tokens_ref,
    gain_ref,
    head_gain_ref,
    rate_ref,
    bias_ref,
    query_hbm,
    key_hbm,
    value_hbm,
    outgate_hbm,
    beta_hbm,
    decay_hbm,
    out_hbm,
    state_hbm,
    mix_ref,
    new_state_hbm,
    proj_buf,
    beta_buf,
    decay_buf,
    out_buf,
    state_buf,
    column_buf,
    readout_buf,
    proj_sem,
    gate_sem,
    out_sem,
    state_sem,
    store_sem,
):
    seq_count = tokens_ref.shape[0]
    head_local, head_size = state_buf.shape[1:3]
    width = head_local * head_size
    chunk_count = seq_count // seq_chunk
    gate_copies = [
        pltpu.make_async_copy(beta_hbm, beta_buf, gate_sem.at[0]),
        pltpu.make_async_copy(decay_hbm, decay_buf, gate_sem.at[1]),
    ]
    proj_copies = [
        pltpu.make_async_copy(hbm, proj_buf.at[i], proj_sem.at[i])
        for i, hbm in enumerate((key_hbm, query_hbm, value_hbm, outgate_hbm))
    ]
    chunks = [pl.ds(c * seq_chunk, seq_chunk) for c in range(chunk_count)]
    state_copies = [
        pltpu.make_async_copy(state_hbm.at[rows], state_buf.at[rows], state_sem.at[c])
        for c, rows in enumerate(chunks)
    ]
    store_copies = [
        pltpu.make_async_copy(state_buf.at[rows], new_state_hbm.at[rows], store_sem.at[c])
        for c, rows in enumerate(chunks)
    ]
    out_copy = pltpu.make_async_copy(out_hbm, out_buf, out_sem.at[0])
    for copy in proj_copies[:3] + gate_copies + state_copies + proj_copies[3:] + [out_copy]:
        copy.start()

    normed = rms_scale(tokens_ref[...].astype(f32), row_of(gain_ref)).astype(bf16)

    def project(index):
        proj_copies[index].wait()
        return dot(normed, proj_buf[index]).astype(bf16).astype(f32)

    def heads_of(raw):
        return [raw[:, h * head_size : (h + 1) * head_size] for h in range(head_local)]

    key_units = [unit_rows(silu(raw)) for raw in heads_of(project(0))]
    query_units = [
        unit_rows(silu(raw)) * head_size ** (-0.5) for raw in heads_of(project(1))
    ]
    value_acts = [silu(raw) for raw in heads_of(project(2))]
    for copy in gate_copies:
        copy.wait()
    beta_all = jax.nn.sigmoid(dot_t(normed, beta_buf[...]))
    decay_all = dot_t(normed, decay_buf[...])
    lane = lax.broadcasted_iota(jnp.int32, beta_all.shape, 1)
    head_start = lax.axis_index("tp") * head_local
    betas, alphas = [], []
    for h in range(head_local):
        chosen = lane == head_start + h
        betas.append(jnp.sum(jnp.where(chosen, beta_all, 0.0), axis=1, keepdims=True))
        raw = jnp.sum(jnp.where(chosen, decay_all, 0.0), axis=1, keepdims=True)
        raw = raw + bias_ref[head_start + h]
        soft = jnp.maximum(raw, 0.0) + jnp.log1p(jnp.exp(-jnp.abs(raw)))
        alphas.append(jnp.exp(-rate_ref[head_start + h] * soft))
    wide = (seq_count, head_size)
    betas = [jnp.broadcast_to(beta, wide) for beta in betas]
    alphas = [jnp.broadcast_to(alpha, wide) for alpha in alphas]
    stacked = jnp.concatenate(key_units + query_units, axis=0)
    short = -stacked.shape[0] % head_size
    if short:
        stacked = jnp.concatenate([stacked, jnp.zeros((short, head_size), f32)], axis=0)
    column_buf[...] = stacked.T
    for c in range(chunk_count):
        state_copies[c].wait()
        for s in range(c * seq_chunk, (c + 1) * seq_chunk):
            for h in range(head_local):
                key_at = h * seq_count + s
                query_at = (head_local + h) * seq_count + s
                key_column = column_buf[:, key_at : key_at + 1]
                query_column = column_buf[:, query_at : query_at + 1]
                alpha = alphas[h][s : s + 1]
                old = state_buf[s, h]
                predicted = alpha * jnp.sum(old * key_column, axis=0, keepdims=True)
                change = betas[h][s : s + 1] * (value_acts[h][s : s + 1] - predicted)
                new = old * alpha + key_column * change
                state_buf[s, h] = new
                readout_buf[s : s + 1, h * head_size : (h + 1) * head_size] = jnp.sum(
                    new * query_column, axis=0, keepdims=True
                )
        store_copies[c].start()
    outgate = project(3)
    gain = row_of(head_gain_ref)
    gated = [rms_scale(part, gain) for part in heads_of(readout_buf[...])]
    gated = (jnp.concatenate(gated, axis=1) * silu(outgate)).astype(bf16)
    out_copy.wait()
    half = mix_ref.shape[2]
    for i in range(mix_ref.shape[0]):
        mix_ref[i] = dot(gated, out_buf[:, i * half : (i + 1) * half]).astype(bf16)
    for copy in store_copies:
        copy.wait()


def expert_kernel(
    ep_count,
    tp_count,
    capacity,
    mix_ref,
    tokens_ref,
    gain_ref,
    blend_ref,
    ids_ref,
    weights_ref,
    dense_gate_hbm,
    dense_up_hbm,
    dense_down_hbm,
    gate_hbm,
    up_hbm,
    down_hbm,
    out_ref,
    wide_buf,
    dense_down_buf,
    down_buf,
    pair_buf,
    chip_buf,
    cross_buf,
    residual_buf,
    part_buf,
    pair_two_buf,
    chip_two_buf,
    cross_two_buf,
    final_buf,
    outgoing_buf,
    arrived_buf,
    result_buf,
    returned_buf,
    rows_buf,
    weight_sem,
    tp_send,
    tp_recv,
    ep_send,
    ep_recv,
):
    seq_count, width = tokens_ref.shape
    half = width // 2
    slot_rows = outgoing_buf.shape[1]
    me = lax.axis_index("ep")
    tp_index = lax.axis_index("tp")
    core = lax.rem(tp_index, 2)
    chip = tp_index // 2
    partner = chip * 2 + 1 - core
    across = lax.rem(chip + 1, 2) * 2 + core

    weight_copies = [
        pltpu.make_async_copy(hbm, buf, weight_sem.at[i])
        for i, (hbm, buf) in enumerate(
            (
                (dense_gate_hbm, wide_buf.at[0]),
                (dense_up_hbm, wide_buf.at[1]),
                (dense_down_hbm, dense_down_buf),
                (gate_hbm.at[0], wide_buf.at[2]),
                (up_hbm.at[0], wide_buf.at[3]),
                (down_hbm.at[0], down_buf),
            )
        )
    ]
    barrier = pltpu.get_barrier_semaphore()
    pl.semaphore_signal(barrier, inc=1, device_id={"tp": partner}, device_id_type=MESH)
    pl.semaphore_signal(barrier, inc=1, device_id={"tp": across}, device_id_type=MESH)

    def greet(step, carry):
        peer = lax.rem(me + step, ep_count)
        pl.semaphore_signal(barrier, inc=1, device_id={"ep": peer}, device_id_type=MESH)
        return carry

    lax.fori_loop(1, ep_count, greet, 0)
    for copy in weight_copies:
        copy.start()
    pl.semaphore_wait(barrier, ep_count + 1)

    def tp_copy(src, dst, index, target):
        return pltpu.make_async_remote_copy(
            src_ref=src,
            dst_ref=dst,
            send_sem=tp_send.at[index],
            recv_sem=tp_recv.at[index],
            device_id={"tp": target},
            device_id_type=MESH,
        )

    def start_pair(source, pair, base):
        copy = tp_copy(source.at[1 - core], pair, base, partner)
        copy.start()
        return copy

    def finish_sum(copy, source, pair, chip_sum, cross, base):
        copy.wait()
        chip_sum[...] = (source[core].astype(f32) + pair[...].astype(f32)).astype(bf16)
        other = tp_copy(chip_sum, cross, base + 1, across)
        other.start()
        other.wait()
        return chip_sum[...].astype(f32) + cross[...].astype(f32)

    def share(buf, base):
        copy = tp_copy(buf.at[core], buf.at[core], base + 2, partner)
        copy.start()
        tp_copy(buf.at[1 - core], buf.at[1 - core], base + 2, partner).wait_recv()
        copy.wait_send()

    first = start_pair(mix_ref, pair_buf, 0)

    expert_count = ep_count * tp_count
    slot_total = ep_count * slot_rows
    ids = ids_ref[...]
    raw_weights = weights_ref[...]
    scales = raw_weights / jnp.sum(raw_weights, axis=0, keepdims=True) * routed_scale
    slot = lax.broadcasted_iota(jnp.int32, (slot_total, seq_count), 0)
    slot_expert = slot // slot_rows * tp_count + tp_index
    slot_place = lax.rem(slot, slot_rows)
    named = jnp.zeros((slot_total, seq_count), f32)
    scale_at = jnp.zeros((slot_total, seq_count), f32)
    for k in range(ids.shape[0]):
        same = ids[k : k + 1] == slot_expert
        named = named + jnp.where(same, 1.0, 0.0)
        scale_at = scale_at + jnp.where(same, scales[k : k + 1], 0.0)
    row = lax.broadcasted_iota(jnp.int32, (seq_count, seq_count), 0)
    col = lax.broadcasted_iota(jnp.int32, (seq_count, seq_count), 1)
    earlier = jnp.where(row < col, 1.0, 0.0).astype(bf16)
    rank = dot(named.astype(bf16), earlier)
    taken = named * jnp.where(rank == slot_place.astype(f32), 1.0, 0.0)
    scale_at = (scale_at * taken).T
    scale_high = scale_at.astype(bf16)
    scale_low = (scale_at - scale_high.astype(f32)).astype(bf16)
    dispatch = taken.astype(bf16)

    mixed = finish_sum(first, mix_ref, pair_buf, chip_buf, cross_buf, 0)
    own_tokens = jnp.where(core == 0, tokens_ref[:, :half].astype(f32), tokens_ref[:, half:].astype(f32))
    residual_buf[core] = (own_tokens + mixed).astype(bf16)
    share(residual_buf, 0)
    residual = jnp.concatenate([residual_buf[0], residual_buf[1]], axis=1).astype(f32)
    normed = rms_scale(residual, row_of(gain_ref)).astype(bf16)
    rows_buf[...] = dot(dispatch, normed)

    def fill(peer, carry):
        block = rows_buf[pl.ds(pl.multiple_of(peer * slot_rows, slot_rows), slot_rows), :]
        outgoing_buf[peer] = block.astype(bf16)
        return carry

    lax.fori_loop(0, ep_count, fill, 0, unroll=ep_count <= 8)

    def ep_copy(src, dst, index, src_at, dst_at, target):
        return pltpu.make_async_remote_copy(
            src_ref=src.at[src_at],
            dst_ref=dst.at[dst_at],
            send_sem=ep_send.at[index, src_at],
            recv_sem=ep_recv.at[index, dst_at],
            device_id={"ep": target},
            device_id_type=MESH,
        )

    def send_all(src, dst, index):
        def step_of(step, carry):
            peer = lax.rem(me + step, ep_count)
            ep_copy(src, dst, index, peer, me, peer).start()
            return carry

        lax.fori_loop(1, ep_count, step_of, 0, unroll=ep_count <= 8)
        dst[me] = src[me]

    def wait_all(src, dst, index):
        def step_of(step, carry):
            peer = lax.rem(me + step, ep_count)
            ep_copy(src, dst, index, peer, peer, peer).wait()
            return carry

        lax.fori_loop(1, ep_count, step_of, 0, unroll=ep_count <= 8)

    def gather_rows(buf):
        def step_of(peer, carry):
            at = pl.ds(pl.multiple_of(peer * slot_rows, slot_rows), slot_rows)
            rows_buf[at, :] = buf[peer].astype(f32)
            return carry

        lax.fori_loop(0, ep_count, step_of, 0, unroll=ep_count <= 8)
        return rows_buf[...].astype(bf16)

    send_all(outgoing_buf, arrived_buf, 0)

    blend_row = row_of(blend_ref)
    blend_gate = jax.nn.sigmoid(
        jnp.sum(normed.astype(f32) * blend_row, axis=1, keepdims=True)
    )
    weight_copies[0].wait()
    dense_gate = dot(normed, wide_buf[0])
    weight_copies[1].wait()
    dense_hidden = (silu(dense_gate) * dot(normed, wide_buf[1])).astype(bf16)
    weight_copies[2].wait()
    dense_part = blend_gate * dot(dense_hidden, dense_down_buf[...])

    wait_all(outgoing_buf, arrived_buf, 0)
    rows = gather_rows(arrived_buf)
    weight_copies[3].wait()
    gate_part = dot(rows, wide_buf[2])
    weight_copies[4].wait()
    hidden = (silu(gate_part) * dot(rows, wide_buf[3])).astype(bf16)
    weight_copies[5].wait()
    rows_buf[...] = dot(hidden, down_buf[...])

    def fill_result(peer, carry):
        block = rows_buf[pl.ds(pl.multiple_of(peer * slot_rows, slot_rows), slot_rows), :]
        result_buf[peer] = block.astype(bf16)
        return carry

    lax.fori_loop(0, ep_count, fill_result, 0, unroll=ep_count <= 8)
    send_all(result_buf, returned_buf, 1)
    wait_all(result_buf, returned_buf, 1)
    rows = gather_rows(returned_buf)
    total = dense_part + dot(scale_high, rows) + dot(scale_low, rows)
    part_buf[0] = total[:, :half].astype(bf16)
    part_buf[1] = total[:, half:].astype(bf16)
    second = start_pair(part_buf, pair_two_buf, 3)
    combined = finish_sum(second, part_buf, pair_two_buf, chip_two_buf, cross_two_buf, 3)
    final_buf[core] = (residual_buf[core].astype(f32) + combined).astype(bf16)
    share(final_buf, 3)
    out_ref[:, :half] = final_buf[0]
    out_ref[:, half:] = final_buf[1]


def shards(
    tokens,
    delta_state,
    first_gain,
    query_weight,
    key_weight,
    value_weight,
    outgate_weight,
    beta_weight,
    decay_weight,
    decay_rate,
    decay_bias,
    head_gain,
    out_weight,
    second_gain,
    blend_weight,
    dense_gate_weight,
    dense_up_weight,
    dense_down_weight,
    expert_gate,
    expert_up,
    expert_down,
    route_ids,
    route_weights,
):
    seq_count, width = tokens.shape
    head_local, head_size = delta_state.shape[1:3]
    ep_count = lax.axis_size("ep")
    tp_count = lax.axis_size("tp")
    half = width // 2
    vmem = pl.BlockSpec(memory_space=pltpu.VMEM)
    smem = pl.BlockSpec(memory_space=pltpu.SMEM)
    hbm = pl.BlockSpec(memory_space=pl.ANY)
    dma = pltpu.SemaphoreType.DMA
    seq_chunk = 4 if seq_count % 4 == 0 else 1
    local_width = query_weight.shape[1]
    stacked = -(-2 * head_local * seq_count // head_size) * head_size
    mix_part, new_state = pl.pallas_call(
        functools.partial(mixer_kernel, seq_chunk),
        out_shape=(
            jax.ShapeDtypeStruct((2, seq_count, half), bf16),
            jax.ShapeDtypeStruct(delta_state.shape, f32),
        ),
        in_specs=[vmem] * 3 + [smem] * 2 + [hbm] * 8,
        out_specs=(vmem, hbm),
        scratch_shapes=[
            pltpu.VMEM((4,) + query_weight.shape, bf16),
            pltpu.VMEM(beta_weight.shape[::-1], bf16),
            pltpu.VMEM(decay_weight.shape[::-1], bf16),
            pltpu.VMEM(out_weight.shape, bf16),
            pltpu.VMEM(delta_state.shape, f32),
            pltpu.VMEM((head_size, stacked), f32),
            pltpu.VMEM((seq_count, local_width), f32),
            dma((4,)),
            dma((2,)),
            dma((1,)),
            dma((seq_count // seq_chunk,)),
            dma((seq_count // seq_chunk,)),
        ],
        compiler_params=pltpu.CompilerParams(vmem_limit_bytes=vmem_bytes),
        name="mixer",
    )(
        tokens,
        first_gain,
        head_gain,
        decay_rate,
        decay_bias,
        query_weight,
        key_weight,
        value_weight,
        outgate_weight,
        beta_weight.T,
        decay_weight.T,
        out_weight,
        delta_state,
    )
    top_count = route_ids.shape[1]
    expert_count = ep_count * tp_count
    capacity = max(2, (3 * seq_count * top_count + 2 * expert_count - 1) // (2 * expert_count))
    slot_rows = -(-capacity // 8) * 8
    wide = pltpu.VMEM((4,) + dense_gate_weight.shape, bf16)
    half_block = pltpu.VMEM((seq_count, half), bf16)
    both_block = pltpu.VMEM((2, seq_count, half), bf16)
    slots = pltpu.VMEM((ep_count, slot_rows, width), bf16)
    new_tokens = pl.pallas_call(
        functools.partial(expert_kernel, ep_count, tp_count, capacity),
        out_shape=jax.ShapeDtypeStruct(tokens.shape, bf16),
        in_specs=[vmem] * 6 + [hbm] * 6,
        out_specs=vmem,
        scratch_shapes=[
            wide,
            pltpu.VMEM(dense_down_weight.shape, bf16),
            pltpu.VMEM(expert_down.shape[1:], bf16),
            half_block,
            half_block,
            half_block,
            both_block,
            both_block,
            half_block,
            half_block,
            half_block,
            both_block,
            slots,
            slots,
            slots,
            slots,
            pltpu.VMEM((ep_count * slot_rows, width), f32),
            dma((6,)),
            dma((6,)),
            dma((6,)),
            dma((2, ep_count)),
            dma((2, ep_count)),
        ],
        compiler_params=pltpu.CompilerParams(
            vmem_limit_bytes=vmem_bytes, collective_id=0, has_side_effects=True
        ),
        name="experts",
    )(
        mix_part,
        tokens,
        second_gain,
        blend_weight,
        route_ids.T,
        route_weights.T,
        dense_gate_weight,
        dense_up_weight,
        dense_down_weight,
        expert_gate,
        expert_up,
        expert_down,
    )
    return (new_tokens, new_state)


def solution(mesh):
    placed = (
        P("ep", None),
        P("ep", "tp", None, None),
        P(),
        P(None, "tp"),
        P(None, "tp"),
        P(None, "tp"),
        P(None, "tp"),
        P(),
        P(),
        P(),
        P(),
        P(),
        P("tp", None),
        P(),
        P(),
        P(None, "tp"),
        P(None, "tp"),
        P("tp", None),
        P(("ep", "tp"), None, None),
        P(("ep", "tp"), None, None),
        P(("ep", "tp"), None, None),
        P("ep", None),
        P("ep", None),
    )
    return jax.shard_map(
        shards,
        mesh=mesh,
        in_specs=placed,
        out_specs=(P("ep", None), P("ep", "tp", None, None)),
        check_vma=False,
    )
```
